32 devices in a mesh: fs: 8 (over z, x), tp: 4 (over y, core).
Axes of the slice: x: 2, y: 2, z: 4, core: 2. Of those that a mesh axis runs over, the one named last changes fastest.
Arguments:
- tokens: bfloat16 [4096, 2048], P('fs', 'tp'), may hold values from -6 to 6
- pre_gain: float32 [2048], P('fs'), may hold values from 0.1 to 1.9
- gate_weight: float32 [2048, 6144], P('fs', 'tp'), may hold values from -0.125 to 0.125
- up_weight: float32 [2048, 6144], P('fs', 'tp'), may hold values from -0.125 to 0.125
- down_weight: float32 [2048, 6144], P('fs', 'tp'), may hold values from -0.078125 to 0.078125
- post_gain: float32 [2048], P('tp'), may hold values from 0.1 to 1.9
Outputs:
- result: bfloat16 [4096, 2048], P('fs', 'tp')
- gate_ready: bfloat16 [2048, 6144], P(None, 'tp')
- up_ready: bfloat16 [2048, 6144], P(None, 'tp')
- down_ready: bfloat16 [2048, 6144], P(None, 'tp')
The draws below stay inside these ranges and needn't reach their ends.
All inputs are finite; a program needn't handle non-finite values.
Results may differ from the reference program's by a relative error of at most 0.015.
Values may be sent and summed in bfloat16 or wider, within the bound.
A program may use at most 128 MiB of HBM per device.

```python
import jax
import jax.numpy as jnp
from jax import lax

D = 2048
FF = 6144
TOKENS = 4096


def levels(rng, shape, pieces, smallest, top_value):
    def one(position, blocks):
        heights = jax.random.uniform(jax.random.fold_in(jax.random.fold_in(rng, 6), position), (blocks,), jnp.float32, smallest / len(pieces), top_value / len(pieces))
        return jnp.repeat(jnp.exp(heights), shape[position] // blocks).reshape((-1,) + (1,) * (len(shape) - position - 1))

    loudness = one(*pieces[0])
    for cut in pieces[1:]:
        loudness = loudness * one(*cut)
    return loudness


def bell_draw(stream_key, extent, spread, reach, cuts=(), kind=jnp.bfloat16):
    drawn = jax.random.normal(stream_key, extent, jnp.float32) * spread
    if len(cuts) > 0:
        drawn = levels(stream_key, extent, cuts, -0.22, 0.18) * drawn
    return jnp.clip(drawn, min=-reach, max=reach).astype(kind)


def setup_inputs(seed: int = 0) -> dict:
    keys = jax.random.split(jax.random.key(seed), 7)
    return {
        "tokens": bell_draw(keys[0], (TOKENS, D), 1.0, 6.0, ((0, 8), (1, 4))),
        "pre_gain": jnp.clip(1.0 + 0.18 * jax.random.normal(keys[1], (D,), jnp.float32), 0.1, 1.9),
        "gate_weight": bell_draw(keys[2], (D, FF), D ** -0.5, 0.125, ((0, 8), (1, 4)), jnp.float32),
        "up_weight": bell_draw(keys[3], (D, FF), D ** -0.5, 0.125, ((0, 8), (1, 4)), jnp.float32),
        "down_weight": bell_draw(keys[4], (D, FF), FF ** -0.5, 0.078125, ((0, 8), (1, 4)), jnp.float32),
        "post_gain": jnp.clip(1.0 + 0.18 * jax.random.normal(keys[5], (D,), jnp.float32), 0.1, 1.9),
    }


EPS = 1e-06

def reference(tokens, pre_gain, gate_weight, up_weight, down_weight, post_gain):
    gate_ready = (pre_gain[:, None] * gate_weight).astype(jnp.bfloat16)
    up_ready = (pre_gain[:, None] * up_weight).astype(jnp.bfloat16)
    down_ready = down_weight.astype(jnp.bfloat16)
    widened = tokens.astype(jnp.float32)
    normalized = (widened * lax.rsqrt(lax.optimization_barrier(jnp.mean(widened * widened, axis=1, keepdims=True)) + EPS)).astype(jnp.bfloat16)
    gate = jnp.dot(normalized, gate_ready, preferred_element_type=jnp.float32)
    up = jnp.dot(normalized, up_ready, preferred_element_type=jnp.float32)
    hidden = (jax.nn.silu(gate) * up).astype(jnp.bfloat16)
    mixed = lax.dot_general(hidden, down_ready, (((1,), (1,)), ((), ())), preferred_element_type=jnp.float32)
    scaling = lax.rsqrt(lax.optimization_barrier(jnp.mean(mixed * mixed, axis=1, keepdims=True)) + EPS)
    result = (mixed * scaling * post_gain[None, :]).astype(jnp.bfloat16)
    return (result, gate_ready, up_ready, down_ready)
```

```python
import functools

import jax
import jax.numpy as jnp
from jax import lax
from jax.experimental import pallas as pl
from jax.experimental.pallas import tpu as pltpu
from jax.sharding import PartitionSpec as P

EPS = 1e-06
MESH = pl.DeviceIdType.MESH
P_PART, Q_PART = 0, 1
UP, DOWN, RIGHT, LEFT = 0, 1, 2, 3
CHUNKS = 4


def kernel(
    fs, tp, lines, cols,
    tokens, pre_gain, gate_weight, up_weight, down_weight, post_gain,
    totals, squares, squares_in, gains_out, gate_out, up_out, down_out,
    staged, gains_row, gains_in, whole, normed, gate, hidden, part, parts_in, powers,
    send_sem, recv_sem, down_recv, stage_sem, gain_sem, tok_send, tok_recv, tok_own,
    rs_send, rs_recv, sq_send, sq_recv,
):
    weights, outs = (gate_weight, up_weight, down_weight), (gate_out, up_out, down_out)
    depth, width = gate_weight.shape
    half = depth // 2
    rows, block = tokens.shape
    me_fs, me = lax.axis_index("fs"), lax.axis_index("tp")
    z, x = me_fs // cols, lax.rem(me_fs, cols)

    sides = {
        UP: (z < lines - 1, me_fs + cols),
        DOWN: (z > 0, me_fs - cols),
        RIGHT: (x < cols - 1, me_fs + 1),
        LEFT: (x > 0, me_fs - 1),
    }
    peers = [lax.rem(me + j, tp) for j in range(1, tp)]
    corner = jnp.logical_or(z == 0, z == lines - 1)

    def describe(m, which, shard, side, target):
        if m < 2:
            ref = outs[m].at[pl.ds(pl.multiple_of(shard * depth, 16), depth), :]
            landed = recv_sem.at[m, shard]
        else:
            ref = outs[2].at[pl.ds(pl.multiple_of(shard * depth + which * half, 16), half), :]
            landed = down_recv.at[which, shard]
        return pltpu.make_async_remote_copy(
            src_ref=ref, dst_ref=ref, send_sem=send_sem.at[m, side], recv_sem=landed,
            device_id={"fs": target, "tp": me}, device_id_type=MESH,
        )

    def send(m, which, shard, side, extra=None):
        there, target = sides[side]
        cond = there if extra is None else jnp.logical_and(there, extra)

        @pl.when(cond)
        def _():
            describe(m, which, shard, side, target).start()

    def arrive(m, which, shard, cond):
        @pl.when(cond)
        def _():
            describe(m, which, shard, 0, lax.rem(me_fs + 1, fs)).wait_recv()

    def sent(m, side, rows_sent):
        ref = outs[m].at[0:rows_sent, :]
        pltpu.make_async_remote_copy(
            src_ref=ref, dst_ref=ref, send_sem=send_sem.at[m, side], recv_sem=recv_sem.at[0, 0],
            device_id={"fs": lax.rem(me_fs + 1, fs), "tp": me}, device_id_type=MESH,
        ).wait_send()

    barrier = pltpu.get_barrier_semaphore()
    for side in sides:
        there, target = sides[side]

        @pl.when(there)
        def _():
            pl.semaphore_signal(barrier, inc=1, device_id={"fs": target, "tp": me}, device_id_type=MESH)

    for peer in peers:
        pl.semaphore_signal(barrier, inc=1, device_id={"fs": me_fs, "tp": peer}, device_id_type=MESH)

    gain_load = pltpu.make_async_copy(pre_gain, gains_row, gain_sem.at[0])
    gain_load.start()
    size = depth // CHUNKS
    for m in range(3):
        for c in range(CHUNKS):
            here = pl.ds(c * size, size)
            pltpu.make_async_copy(weights[m].at[here, :], staged.at[m, here, :], stage_sem.at[m]).start()
    own_tokens = pltpu.make_async_copy(tokens, whole.at[me], tok_own)
    own_tokens.start()
    post_load = pltpu.make_async_copy(post_gain, gains_out, gain_sem.at[1])
    post_load.start()
    gain_load.wait()
    gains_in[...] = jnp.transpose(jnp.broadcast_to(gains_row[0:1, :], (128, depth)))

    def cast(m):
        pltpu.make_async_copy(weights[m], staged.at[m], stage_sem.at[m]).wait()

        @pl.loop(0, depth // 16)
        def _(i):
            here = pl.ds(pl.multiple_of(i * 16, 16), 16)
            v = staged[m, here, :]
            if m < 2:
                v = gains_in[here, 0:1] * v
            outs[m][pl.ds(pl.multiple_of(me_fs * depth + i * 16, 16), 16), :] = v.astype(jnp.bfloat16)

    def token_copy(j):
        return pltpu.make_async_remote_copy(
            src_ref=tokens, dst_ref=whole.at[me], send_sem=tok_send, recv_sem=tok_recv,
            device_id={"fs": me_fs, "tp": peers[j]}, device_id_type=MESH,
        )

    def token_all():
        ref = whole.at[0:tp - 1]
        return pltpu.make_async_remote_copy(
            src_ref=ref, dst_ref=ref, send_sem=tok_send, recv_sem=tok_recv,
            device_id={"fs": me_fs, "tp": peers[0]}, device_id_type=MESH,
        )

    cast(0)
    pl.semaphore_wait(barrier, tp - 1 + sum(there.astype(jnp.int32) for there, _ in sides.values()))
    for side in sides:
        send(0, Q_PART, me_fs, side)
    for j in range(tp - 1):
        token_copy(j).start()
    cast(1)
    for side in sides:
        send(1, Q_PART, me_fs, side)
    cast(2)
    for side in (RIGHT, LEFT):
        send(2, P_PART, me_fs, side)

    def normalize():
        own_tokens.wait()
        token_all().wait_recv()
        step = 64

        @pl.loop(0, rows // step)
        def _(i):
            here = pl.ds(pl.multiple_of(i * step, step), step)
            total = jnp.zeros((step, 1), jnp.float32)
            for t in range(tp):
                v = whole[t, here, :].astype(jnp.float32)
                total = total + jnp.sum(v * v, axis=1, keepdims=True)
            scale = lax.rsqrt(total / (tp * block) + EPS)
            for t in range(tp):
                v = whole[t, here, :].astype(jnp.float32)
                normed[here, t * block:(t + 1) * block] = (v * scale).astype(jnp.bfloat16)

    def valid(line):
        return jnp.logical_and(line >= 0, line < lines)

    def around(s):
        return (UP, z - 1 - s), (DOWN, z + 1 + s)

    def along_x(m, which, line, cond=None):
        for r in range(cols - 1):
            for side, column in ((RIGHT, x - 1 - r), (LEFT, x + 1 + r)):
                there = jnp.logical_and(column >= 0, column < cols)
                if cond is not None:
                    there = jnp.logical_and(there, cond)
                arrive(m, which, line * cols + column, there)
                if r < cols - 2:
                    send(m, which, line * cols + column, side, there)

    def along_z(m, s):
        for side, line in around(s):
            there = valid(line)
            shard = line * cols + x
            arrive(m, Q_PART, shard, there)
            if s < lines - 2:
                send(m, Q_PART, shard, side, there)
            if m < 2:
                send(m, Q_PART, shard, RIGHT, there)
                send(m, Q_PART, shard, LEFT, there)

    final = {UP: jnp.minimum(me, lines - 2), DOWN: jnp.maximum(me, 1)}
    next_to_end = {UP: z == lines - 2, DOWN: z == 1}

    def put_off(side, line):
        return jnp.logical_and(next_to_end[side], line == final[side])

    def own_down(s):
        for side, behind in ((UP, z), (DOWN, lines - 1 - z)):
            now = behind <= 1 if s == 0 else behind == s + 1
            send(2, Q_PART, me_fs, side, now)
            now = jnp.logical_and(now, jnp.logical_not(put_off(side, z)))
            for c in range(cols):
                send(2, P_PART, z * cols + lax.rem(x + c, cols), side, now)

    def pass_p(s):
        for side, line in around(s):
            there = jnp.logical_and(valid(line), sides[side][0])
            on = jnp.logical_not(put_off(side, line))
            for c in range(cols):
                shard = line * cols + lax.rem(x + c, cols)
                arrive(2, P_PART, shard, there)
                send(2, P_PART, shard, side, jnp.logical_and(there, on))

    for s in range(lines - 1):
        for m in range(2):
            along_z(m, s)
        if s == 0:
            along_x(2, P_PART, z)
        own_down(s)
        if s == 0:
            normalize()
    for s in range(lines - 1):
        along_z(2, s)

    def in_turn(i):
        return me if i is None else jnp.where(i < me, i, i + 1)

    for i in list(range(lines - 1)) + [None]:
        for side in (RIGHT, LEFT):
            send(2, Q_PART, in_turn(i) * cols + x, side)
    for s in range(lines - 2):
        pass_p(s)
    for side in (UP, DOWN):
        for c in range(cols):
            send(2, P_PART, final[side] * cols + lax.rem(x + c, cols), side, next_to_end[side])

    tile = 256

    def project(m):
        along_x(m, Q_PART, z)
        for s in range(lines - 1):
            for _, line in around(s):
                along_x(m, Q_PART, line, valid(line))

        @pl.loop(0, width // tile)
        def _(i):
            here = pl.ds(pl.multiple_of(i * tile, tile), tile)
            product = jnp.dot(normed[...], outs[m][:, here], preferred_element_type=jnp.float32)
            if m == 0:
                gate[:, here] = product
            else:
                g = gate[:, here]
                hidden[:, here] = (g / (1.0 + jnp.exp(-g)) * product).astype(jnp.bfloat16)

    def share_copy(line, column, which):
        return pltpu.make_async_remote_copy(
            src_ref=part.at[line, column, which], dst_ref=parts_in.at[me, column, which],
            send_sem=rs_send, recv_sem=rs_recv.at[column, which],
            device_id={"fs": me_fs, "tp": line}, device_id_type=MESH,
        )

    def mix(line, column, which):
        here = pl.ds(pl.multiple_of((line * cols + column) * depth + which * half, 16), half)
        product = lax.dot_general(
            hidden[...], outs[2][here, :], (((1,), (1,)), ((), ())), preferred_element_type=jnp.float32
        )
        part[line, column, which] = product.astype(jnp.bfloat16)

        @pl.when(line != me)
        def _():
            share_copy(line, column, which).start()

    def mix_columns(line, which, first, cond=None):
        @pl.loop(first, cols)
        def _(c):
            if cond is None:
                mix(line, lax.rem(x + c, cols), which)
            else:
                pl.when(cond)(lambda: mix(line, lax.rem(x + c, cols), which))

    def add_up(column, which, first=False):
        ref = parts_in.at[0:tp - 1, column, which]
        pltpu.make_async_remote_copy(
            src_ref=ref, dst_ref=ref, send_sem=rs_send, recv_sem=rs_recv.at[column, which],
            device_id={"fs": me_fs, "tp": peers[0]}, device_id_type=MESH,
        ).wait_recv()
        step = 128

        @pl.loop(0, rows // step)
        def _(i):
            here = pl.ds(pl.multiple_of(i * step, step), step)
            total = part[me, column, which, here, :].astype(jnp.float32)
            for peer in peers:
                total = total + parts_in[peer, column, which, here, :].astype(jnp.float32)
            totals[column, which, here, :] = total
            powers[here, :] = total * total if first else powers[here, :] + total * total

    project(0)
    project(1)

    @pl.loop(0, lines)
    def _(line):
        mix(line, x, Q_PART)

    @pl.loop(0, lines)
    def _(line):
        mix_columns(line, P_PART, 0, jnp.logical_or(line == z, jnp.logical_not(corner)))

    inward = jnp.where(z == 0, 1, -1)
    last_p = jnp.where(z == 0, final[DOWN], final[UP])
    last_gap = (last_p - z) * inward

    def late_p(n):
        gap = n // cols + 1
        gap = jnp.where(gap < last_gap, gap, jnp.where(gap < lines - 1, gap + 1, last_gap))
        line, column = z + inward * gap, lax.rem(x + lax.rem(n, cols), cols)

        @pl.when(corner)
        def _():
            arrive(2, P_PART, line * cols + column, corner)
            mix(line, column, P_PART)

    def late_q(line):
        along_x(2, Q_PART, line)
        mix_columns(line, Q_PART, 1)

    ends, turns = (lines - 1) * cols, lines
    lead = max(0, ends - turns)

    @pl.loop(0, lead)
    def _(n):
        late_p(n)

    @pl.loop(0, ends - lead - 1)
    def _(n):
        late_p(lead + n)
        late_q(jnp.where(n < me, n, n + 1))

    add_up(x, Q_PART, True)
    for c in range(cols - 1):
        add_up(lax.rem(x + c, cols), P_PART)
    late_p(jnp.int32(ends - 1))
    late_q(me)
    add_up(lax.rem(x + cols - 1, cols), P_PART)
    for c in range(1, cols):
        add_up(lax.rem(x + c, cols), Q_PART)
    step = 128

    @pl.loop(0, rows // step)
    def _(i):
        here = pl.ds(pl.multiple_of(i * step, step), step)
        square = jnp.sum(powers[here, :], axis=1, keepdims=True)
        squares[:, here] = jnp.transpose(jnp.broadcast_to(square, (step, 128)))[0:8, :]

    def square_copy(j):
        return pltpu.make_async_remote_copy(
            src_ref=squares, dst_ref=squares_in.at[j], send_sem=sq_send, recv_sem=sq_recv.at[j],
            device_id={"fs": me_fs, "tp": peers[j]}, device_id_type=MESH,
        )

    for j in range(tp - 1):
        square_copy(j).start()
    for n in range(1, lines):
        for m in range(3):
            each = depth if m < 2 else (1 + cols) * half
            pl.when(z + 1 == n)(lambda: sent(m, UP, n * each))
            pl.when(lines - z == n)(lambda: sent(m, DOWN, n * each))
    for n in range(1, cols):
        for m in range(3):
            each = lines * depth if m < 2 else (lines + 1) * half
            pl.when(x + 1 == n)(lambda: sent(m, RIGHT, n * each))
            pl.when(cols - x == n)(lambda: sent(m, LEFT, n * each))
    token_all().wait_send()
    post_load.wait()
    ref = parts_in.at[0:tp - 1]
    pltpu.make_async_remote_copy(
        src_ref=ref, dst_ref=ref, send_sem=rs_send, recv_sem=rs_recv.at[0, 0],
        device_id={"fs": me_fs, "tp": peers[0]}, device_id_type=MESH,
    ).wait_send()
    for j in range(tp - 1):
        square_copy(j).wait_recv()
    pltpu.make_async_remote_copy(
        src_ref=squares_in, dst_ref=squares_in, send_sem=sq_send, recv_sem=sq_recv.at[0],
        device_id={"fs": me_fs, "tp": peers[0]}, device_id_type=MESH,
    ).wait_send()


def write_out(
    width, totals, squares, squares_in, gains, gate_held, up_held, down_held,
    result_out, gate_out, up_out, down_out, result, sems, last,
):
    copies = []
    for k, (ref, out) in enumerate(((gate_held, gate_out), (up_held, up_out), (down_held, down_out))):
        size = ref.shape[0] // CHUNKS
        for c in range(CHUNKS):
            here = pl.ds(c * size, size)
            copies.append(pltpu.make_async_copy(ref.at[here, :], out.at[here, :], sems.at[k, c]))
    for c in copies:
        c.start()
    rows, block = result.shape
    cols, _, _, half = totals.shape
    step = 128

    @pl.loop(0, rows // step)
    def _(i):
        here = pl.ds(pl.multiple_of(i * step, step), step)
        total = squares[:, here]
        for j in range(squares_in.shape[0]):
            total = total + squares_in[j, :, here]
        total = jnp.broadcast_to(total[0:1, :], (128, step))
        scale = lax.rsqrt(jnp.transpose(total)[:, 0:1] / width + EPS)
        for c in range(cols):
            for which in range(2):
                at = slice((2 * c + which) * half, (2 * c + which + 1) * half)
                result[here, at] = (totals[c, which, here, :] * scale * gains[0:1, at]).astype(jnp.bfloat16)

    final = pltpu.make_async_copy(result, result_out, last)
    final.start()
    for c in copies:
        c.wait()
    final.wait()


def solution(mesh):
    fs, tp = mesh.shape["fs"], mesh.shape["tp"]
    lines, cols = tp, fs // tp

    def shards(tokens, pre_gain, gate_weight, up_weight, down_weight, post_gain):
        depth, width = gate_weight.shape
        rows, block = tokens.shape
        hbm = pl.BlockSpec(memory_space=pltpu.HBM)
        vmem = pl.BlockSpec(memory_space=pltpu.VMEM)
        dma = pltpu.SemaphoreType.DMA
        half = depth // 2
        shapes = [(rows, block)] + [(fs * depth, width)] * 3
        held = pl.pallas_call(
            functools.partial(kernel, fs, tp, lines, cols),
            out_shape=(
                pltpu.VMEM((cols, 2, rows, half), jnp.float32),
                pltpu.VMEM((8, rows), jnp.float32),
                pltpu.VMEM((tp - 1, 8, rows), jnp.float32),
                pltpu.VMEM((1, block), jnp.float32),
            ) + tuple(pltpu.VMEM(s, jnp.bfloat16) for s in shapes[1:]),
            in_specs=[hbm] * 6,
            out_specs=(vmem,) * 7,
            scratch_shapes=[
                pltpu.VMEM((3, depth, width), jnp.float32),
                pltpu.VMEM((1, depth), jnp.float32),
                pltpu.VMEM((depth, 128), jnp.float32),
                pltpu.VMEM((tp, rows, block), jnp.bfloat16),
                pltpu.VMEM((rows, tp * block), jnp.bfloat16),
                pltpu.VMEM((rows, width), jnp.float32),
                pltpu.VMEM((rows, width), jnp.bfloat16),
                pltpu.VMEM((tp, cols, 2, rows, half), jnp.bfloat16),
                pltpu.VMEM((tp, cols, 2, rows, half), jnp.bfloat16),
                pltpu.VMEM((rows, half), jnp.float32),
                dma((3, 4)), dma((2, fs)), dma((2, fs)), dma((3,)), dma((2,)), dma, dma, dma,
                dma, dma((cols, 2)), dma, dma((tp - 1,)),
            ],
            compiler_params=pltpu.CompilerParams(collective_id=0, has_side_effects=True, vmem_limit_bytes=42 * 1024 * 1024),
        )(tokens, pre_gain[None, :], gate_weight, up_weight, down_weight, post_gain[None, :])
        return tuple(pl.pallas_call(
            functools.partial(write_out, tp * block),
            out_shape=tuple(jax.ShapeDtypeStruct(s, jnp.bfloat16) for s in shapes),
            in_specs=[vmem] * 7,
            out_specs=(hbm,) * 4,
            scratch_shapes=[pltpu.VMEM((rows, block), jnp.bfloat16), dma((3, CHUNKS)), dma],
            compiler_params=pltpu.CompilerParams(vmem_limit_bytes=2 * 1024 * 1024),
        )(*held))

    return jax.shard_map(
        shards,
        mesh=mesh,
        in_specs=(P("fs", "tp"), P("fs"), P("fs", "tp"), P("fs", "tp"), P("fs", "tp"), P("tp")),
        out_specs=(P("fs", "tp"), P(None, "tp"), P(None, "tp"), P(None, "tp")),
        check_vma=False,
    )
```

```python
import functools

import jax
import jax.numpy as jnp
from jax import lax
from jax.experimental import pallas as pl
from jax.experimental.pallas import tpu as pltpu
from jax.sharding import PartitionSpec as P

EPS = 1e-06
MESH = pl.DeviceIdType.MESH
P_PART, Q_PART = 0, 1
UP, DOWN, RIGHT, LEFT = 0, 1, 2, 3
CHUNKS = 4


def kernel(
    fs, tp, lines, cols,
    tokens, pre_gain, gate_weight, up_weight, down_weight, post_gain,
    totals, squares, squares_in, gains_out, gate_out, up_out, down_out,
    staged, gains_row, gains_in, whole, normed, gate, hidden, part, parts_in, powers,
    send_sem, recv_sem, down_recv, stage_sem, gain_sem, tok_send, tok_recv, tok_own,
    rs_send, rs_recv, sq_send, sq_recv,
):
    weights, outs = (gate_weight, up_weight, down_weight), (gate_out, up_out, down_out)
    depth, width = gate_weight.shape
    half = depth // 2
    rows, block = tokens.shape
    me_fs, me = lax.axis_index("fs"), lax.axis_index("tp")
    z, x = me_fs // cols, lax.rem(me_fs, cols)

    sides = {
        UP: (z < lines - 1, me_fs + cols),
        DOWN: (z > 0, me_fs - cols),
        RIGHT: (x < cols - 1, me_fs + 1),
        LEFT: (x > 0, me_fs - 1),
    }
    peers = [lax.rem(me + j, tp) for j in range(1, tp)]
    corner = jnp.logical_or(z == 0, z == lines - 1)

    def describe(m, which, shard, side, target):
        if m < 2:
            ref = outs[m].at[pl.ds(pl.multiple_of(shard * depth, 16), depth), :]
            landed = recv_sem.at[m, shard]
        else:
            ref = outs[2].at[pl.ds(pl.multiple_of(shard * depth + which * half, 16), half), :]
            landed = down_recv.at[which, shard]
        return pltpu.make_async_remote_copy(
            src_ref=ref, dst_ref=ref, send_sem=send_sem.at[m, side], recv_sem=landed,
            device_id={"fs": target, "tp": me}, device_id_type=MESH,
        )

    def send(m, which, shard, side, extra=None):
        there, target = sides[side]
        cond = there if extra is None else jnp.logical_and(there, extra)

        @pl.when(cond)
        def _():
            describe(m, which, shard, side, target).start()

    def arrive(m, which, shard, cond):
        @pl.when(cond)
        def _():
            describe(m, which, shard, 0, lax.rem(me_fs + 1, fs)).wait_recv()

    def sent(m, side, rows_sent):
        ref = outs[m].at[0:rows_sent, :]
        pltpu.make_async_remote_copy(
            src_ref=ref, dst_ref=ref, send_sem=send_sem.at[m, side], recv_sem=recv_sem.at[0, 0],
            device_id={"fs": lax.rem(me_fs + 1, fs), "tp": me}, device_id_type=MESH,
        ).wait_send()

    barrier = pltpu.get_barrier_semaphore()
    for side in sides:
        there, target = sides[side]

        @pl.when(there)
        def _():
            pl.semaphore_signal(barrier, inc=1, device_id={"fs": target, "tp": me}, device_id_type=MESH)

    for peer in peers:
        pl.semaphore_signal(barrier, inc=1, device_id={"fs": me_fs, "tp": peer}, device_id_type=MESH)

    gain_load = pltpu.make_async_copy(pre_gain, gains_row, gain_sem.at[0])
    gain_load.start()
    size = depth // CHUNKS

    def load(m, c):
        here = pl.ds(c * size, size)
        sem = stage_sem.at[c] if m == 0 else stage_sem.at[CHUNKS + m - 1]
        return pltpu.make_async_copy(weights[m].at[here, :], staged.at[m, here, :], sem)

    for c in range(CHUNKS):
        load(0, c).start()
    own_tokens = pltpu.make_async_copy(tokens, whole.at[me], tok_own)
    post_load = pltpu.make_async_copy(post_gain, gains_out, gain_sem.at[1])
    gain_load.wait()
    gains_in[...] = jnp.transpose(jnp.broadcast_to(gains_row[0:1, :], (128, depth)))

    def cast(m, start, size):
        @pl.loop(start // 16, (start + size) // 16)
        def _(i):
            here = pl.ds(pl.multiple_of(i * 16, 16), 16)
            v = staged[m, here, :]
            if m < 2:
                v = gains_in[here, 0:1] * v
            outs[m][pl.ds(pl.multiple_of(me_fs * depth + i * 16, 16), 16), :] = v.astype(jnp.bfloat16)

    def cast_all(m):
        pltpu.make_async_copy(weights[m], staged.at[m], stage_sem.at[CHUNKS + m - 1]).wait()
        cast(m, 0, depth)

    def token_copy(j):
        return pltpu.make_async_remote_copy(
            src_ref=tokens, dst_ref=whole.at[me], send_sem=tok_send, recv_sem=tok_recv,
            device_id={"fs": me_fs, "tp": peers[j]}, device_id_type=MESH,
        )

    def token_all():
        ref = whole.at[0:tp - 1]
        return pltpu.make_async_remote_copy(
            src_ref=ref, dst_ref=ref, send_sem=tok_send, recv_sem=tok_recv,
            device_id={"fs": me_fs, "tp": peers[0]}, device_id_type=MESH,
        )

    for c in range(CHUNKS):
        load(0, c).wait()
        cast(0, c * size, size)
        if c == 0:
            for m in (1, 2):
                for k in range(CHUNKS):
                    load(m, k).start()
            own_tokens.start()
            post_load.start()
            pl.semaphore_wait(barrier, tp - 1 + sum(there.astype(jnp.int32) for there, _ in sides.values()))
        ref = gate_out.at[pl.ds(pl.multiple_of(me_fs * depth + c * size, 16), size), :]
        for side, (there, target) in sides.items():
            @pl.when(there)
            def _():
                pltpu.make_async_remote_copy(
                    src_ref=ref, dst_ref=ref, send_sem=send_sem.at[0, side], recv_sem=recv_sem.at[0, me_fs],
                    device_id={"fs": target, "tp": me}, device_id_type=MESH,
                ).start()

    for j in range(tp - 1):
        token_copy(j).start()
    cast_all(1)
    for side in sides:
        send(1, Q_PART, me_fs, side)
    cast_all(2)
    for side in (RIGHT, LEFT):
        send(2, P_PART, me_fs, side)

    def normalize():
        own_tokens.wait()
        token_all().wait_recv()
        step = 64

        @pl.loop(0, rows // step)
        def _(i):
            here = pl.ds(pl.multiple_of(i * step, step), step)
            total = jnp.zeros((step, 1), jnp.float32)
            for t in range(tp):
                v = whole[t, here, :].astype(jnp.float32)
                total = total + jnp.sum(v * v, axis=1, keepdims=True)
            scale = lax.rsqrt(total / (tp * block) + EPS)
            for t in range(tp):
                v = whole[t, here, :].astype(jnp.float32)
                normed[here, t * block:(t + 1) * block] = (v * scale).astype(jnp.bfloat16)

    def valid(line):
        return jnp.logical_and(line >= 0, line < lines)

    def around(s):
        return (UP, z - 1 - s), (DOWN, z + 1 + s)

    def along_x(m, which, line, cond=None):
        for r in range(cols - 1):
            for side, column in ((RIGHT, x - 1 - r), (LEFT, x + 1 + r)):
                there = jnp.logical_and(column >= 0, column < cols)
                if cond is not None:
                    there = jnp.logical_and(there, cond)
                arrive(m, which, line * cols + column, there)
                if r < cols - 2:
                    send(m, which, line * cols + column, side, there)

    def along_z(m, s):
        for side, line in around(s):
            there = valid(line)
            shard = line * cols + x
            arrive(m, Q_PART, shard, there)
            if s < lines - 2:
                send(m, Q_PART, shard, side, there)
            if m < 2:
                send(m, Q_PART, shard, RIGHT, there)
                send(m, Q_PART, shard, LEFT, there)

    final = {UP: jnp.minimum(me, lines - 2), DOWN: jnp.maximum(me, 1)}
    next_to_end = {UP: z == lines - 2, DOWN: z == 1}

    def put_off(side, line):
        return jnp.logical_and(next_to_end[side], line == final[side])

    def own_down(s):
        for side, behind in ((UP, z), (DOWN, lines - 1 - z)):
            now = behind <= 1 if s == 0 else behind == s + 1
            send(2, Q_PART, me_fs, side, now)
            now = jnp.logical_and(now, jnp.logical_not(put_off(side, z)))
            for c in range(cols):
                send(2, P_PART, z * cols + lax.rem(x + c, cols), side, now)

    def pass_p(s):
        for side, line in around(s):
            there = jnp.logical_and(valid(line), sides[side][0])
            on = jnp.logical_not(put_off(side, line))
            for c in range(cols):
                shard = line * cols + lax.rem(x + c, cols)
                arrive(2, P_PART, shard, there)
                send(2, P_PART, shard, side, jnp.logical_and(there, on))

    for s in range(lines - 1):
        for m in range(2):
            along_z(m, s)
        if s == 0:
            along_x(2, P_PART, z)
        own_down(s)
        if s == 0:
            normalize()
    for s in range(lines - 1):
        along_z(2, s)

    def in_turn(i):
        return me if i is None else jnp.where(i < me, i, i + 1)

    for i in list(range(lines - 1)) + [None]:
        for side in (RIGHT, LEFT):
            send(2, Q_PART, in_turn(i) * cols + x, side)
    for s in range(lines - 2):
        pass_p(s)
    for side in (UP, DOWN):
        for c in range(cols):
            send(2, P_PART, final[side] * cols + lax.rem(x + c, cols), side, next_to_end[side])

    tile = 256

    def project(m):
        along_x(m, Q_PART, z)
        for s in range(lines - 1):
            for _, line in around(s):
                along_x(m, Q_PART, line, valid(line))

        @pl.loop(0, width // tile)
        def _(i):
            here = pl.ds(pl.multiple_of(i * tile, tile), tile)
            product = jnp.dot(normed[...], outs[m][:, here], preferred_element_type=jnp.float32)
            if m == 0:
                gate[:, here] = product
            else:
                g = gate[:, here]
                hidden[:, here] = (g / (1.0 + jnp.exp(-g)) * product).astype(jnp.bfloat16)

    def share_copy(line, column, which):
        return pltpu.make_async_remote_copy(
            src_ref=part.at[line, column, which], dst_ref=parts_in.at[me, column, which],
            send_sem=rs_send, recv_sem=rs_recv.at[column, which],
            device_id={"fs": me_fs, "tp": line}, device_id_type=MESH,
        )

    def mix(line, column, which):
        here = pl.ds(pl.multiple_of((line * cols + column) * depth + which * half, 16), half)
        product = lax.dot_general(
            hidden[...], outs[2][here, :], (((1,), (1,)), ((), ())), preferred_element_type=jnp.float32
        )
        part[line, column, which] = product.astype(jnp.bfloat16)

        @pl.when(line != me)
        def _():
            share_copy(line, column, which).start()

    def mix_columns(line, which, first, cond=None):
        @pl.loop(first, cols)
        def _(c):
            if cond is None:
                mix(line, lax.rem(x + c, cols), which)
            else:
                pl.when(cond)(lambda: mix(line, lax.rem(x + c, cols), which))

    def add_up(column, which, first=False):
        ref = parts_in.at[0:tp - 1, column, which]
        pltpu.make_async_remote_copy(
            src_ref=ref, dst_ref=ref, send_sem=rs_send, recv_sem=rs_recv.at[column, which],
            device_id={"fs": me_fs, "tp": peers[0]}, device_id_type=MESH,
        ).wait_recv()
        step = 128

        @pl.loop(0, rows // step)
        def _(i):
            here = pl.ds(pl.multiple_of(i * step, step), step)
            total = part[me, column, which, here, :].astype(jnp.float32)
            for peer in peers:
                total = total + parts_in[peer, column, which, here, :].astype(jnp.float32)
            totals[column, which, here, :] = total
            powers[here, :] = total * total if first else powers[here, :] + total * total

    project(0)
    project(1)

    @pl.loop(0, lines)
    def _(line):
        mix(line, x, Q_PART)

    @pl.loop(0, lines)
    def _(line):
        mix_columns(line, P_PART, 0, jnp.logical_or(line == z, jnp.logical_not(corner)))

    inward = jnp.where(z == 0, 1, -1)
    last_p = jnp.where(z == 0, final[DOWN], final[UP])
    last_gap = (last_p - z) * inward

    def late_p(n):
        gap = n // cols + 1
        gap = jnp.where(gap < last_gap, gap, jnp.where(gap < lines - 1, gap + 1, last_gap))
        line, column = z + inward * gap, lax.rem(x + lax.rem(n, cols), cols)

        @pl.when(corner)
        def _():
            arrive(2, P_PART, line * cols + column, corner)
            mix(line, column, P_PART)

    def late_q(line):
        along_x(2, Q_PART, line)
        mix_columns(line, Q_PART, 1)

    ends, turns = (lines - 1) * cols, lines
    lead = max(0, ends - turns)

    @pl.loop(0, lead)
    def _(n):
        late_p(n)

    @pl.loop(0, ends - lead - 1)
    def _(n):
        late_p(lead + n)
        late_q(jnp.where(n < me, n, n + 1))

    add_up(x, Q_PART, True)
    for c in range(cols - 1):
        add_up(lax.rem(x + c, cols), P_PART)
    late_p(jnp.int32(ends - 1))
    late_q(me)
    add_up(lax.rem(x + cols - 1, cols), P_PART)
    for c in range(1, cols):
        add_up(lax.rem(x + c, cols), Q_PART)
    step = 128

    @pl.loop(0, rows // step)
    def _(i):
        here = pl.ds(pl.multiple_of(i * step, step), step)
        square = jnp.sum(powers[here, :], axis=1, keepdims=True)
        squares[:, here] = jnp.transpose(jnp.broadcast_to(square, (step, 128)))[0:8, :]

    def square_copy(j):
        return pltpu.make_async_remote_copy(
            src_ref=squares, dst_ref=squares_in.at[j], send_sem=sq_send, recv_sem=sq_recv.at[j],
            device_id={"fs": me_fs, "tp": peers[j]}, device_id_type=MESH,
        )

    for j in range(tp - 1):
        square_copy(j).start()
    for n in range(1, lines):
        for m in range(3):
            each = depth if m < 2 else (1 + cols) * half
            pl.when(z + 1 == n)(lambda: sent(m, UP, n * each))
            pl.when(lines - z == n)(lambda: sent(m, DOWN, n * each))
    for n in range(1, cols):
        for m in range(3):
            each = lines * depth if m < 2 else (lines + 1) * half
            pl.when(x + 1 == n)(lambda: sent(m, RIGHT, n * each))
            pl.when(cols - x == n)(lambda: sent(m, LEFT, n * each))
    token_all().wait_send()
    post_load.wait()
    ref = parts_in.at[0:tp - 1]
    pltpu.make_async_remote_copy(
        src_ref=ref, dst_ref=ref, send_sem=rs_send, recv_sem=rs_recv.at[0, 0],
        device_id={"fs": me_fs, "tp": peers[0]}, device_id_type=MESH,
    ).wait_send()
    for j in range(tp - 1):
        square_copy(j).wait_recv()
    pltpu.make_async_remote_copy(
        src_ref=squares_in, dst_ref=squares_in, send_sem=sq_send, recv_sem=sq_recv.at[0],
        device_id={"fs": me_fs, "tp": peers[0]}, device_id_type=MESH,
    ).wait_send()


def write_out(
    width, totals, squares, squares_in, gains, gate_held, up_held, down_held,
    result_out, gate_out, up_out, down_out, result, sems, last,
):
    copies = []
    for k, (ref, out) in enumerate(((gate_held, gate_out), (up_held, up_out), (down_held, down_out))):
        size = ref.shape[0] // CHUNKS
        for c in range(CHUNKS):
            here = pl.ds(c * size, size)
            copies.append(pltpu.make_async_copy(ref.at[here, :], out.at[here, :], sems.at[k, c]))
    for c in copies:
        c.start()
    rows, block = result.shape
    cols, _, _, half = totals.shape
    step = 128

    @pl.loop(0, rows // step)
    def _(i):
        here = pl.ds(pl.multiple_of(i * step, step), step)
        total = squares[:, here]
        for j in range(squares_in.shape[0]):
            total = total + squares_in[j, :, here]
        total = jnp.broadcast_to(total[0:1, :], (128, step))
        scale = lax.rsqrt(jnp.transpose(total)[:, 0:1] / width + EPS)
        for c in range(cols):
            for which in range(2):
                at = slice((2 * c + which) * half, (2 * c + which + 1) * half)
                result[here, at] = (totals[c, which, here, :] * scale * gains[0:1, at]).astype(jnp.bfloat16)

    final = pltpu.make_async_copy(result, result_out, last)
    final.start()
    for c in copies:
        c.wait()
    final.wait()


def solution(mesh):
    fs, tp = mesh.shape["fs"], mesh.shape["tp"]
    lines, cols = tp, fs // tp

    def shards(tokens, pre_gain, gate_weight, up_weight, down_weight, post_gain):
        depth, width = gate_weight.shape
        rows, block = tokens.shape
        hbm = pl.BlockSpec(memory_space=pltpu.HBM)
        vmem = pl.BlockSpec(memory_space=pltpu.VMEM)
        dma = pltpu.SemaphoreType.DMA
        half = depth // 2
        shapes = [(rows, block)] + [(fs * depth, width)] * 3
        held = pl.pallas_call(
            functools.partial(kernel, fs, tp, lines, cols),
            out_shape=(
                pltpu.VMEM((cols, 2, rows, half), jnp.float32),
                pltpu.VMEM((8, rows), jnp.float32),
                pltpu.VMEM((tp - 1, 8, rows), jnp.float32),
                pltpu.VMEM((1, block), jnp.float32),
            ) + tuple(pltpu.VMEM(s, jnp.bfloat16) for s in shapes[1:]),
            in_specs=[hbm] * 6,
            out_specs=(vmem,) * 7,
            scratch_shapes=[
                pltpu.VMEM((3, depth, width), jnp.float32),
                pltpu.VMEM((1, depth), jnp.float32),
                pltpu.VMEM((depth, 128), jnp.float32),
                pltpu.VMEM((tp, rows, block), jnp.bfloat16),
                pltpu.VMEM((rows, tp * block), jnp.bfloat16),
                pltpu.VMEM((rows, width), jnp.float32),
                pltpu.VMEM((rows, width), jnp.bfloat16),
                pltpu.VMEM((tp, cols, 2, rows, half), jnp.bfloat16),
                pltpu.VMEM((tp, cols, 2, rows, half), jnp.bfloat16),
                pltpu.VMEM((rows, half), jnp.float32),
                dma((3, 4)), dma((2, fs)), dma((2, fs)), dma((CHUNKS + 2,)), dma((2,)), dma, dma, dma,
                dma, dma((cols, 2)), dma, dma((tp - 1,)),
            ],
            compiler_params=pltpu.CompilerParams(collective_id=0, has_side_effects=True, vmem_limit_bytes=42 * 1024 * 1024),
        )(tokens, pre_gain[None, :], gate_weight, up_weight, down_weight, post_gain[None, :])
        return tuple(pl.pallas_call(
            functools.partial(write_out, tp * block),
            out_shape=tuple(jax.ShapeDtypeStruct(s, jnp.bfloat16) for s in shapes),
            in_specs=[vmem] * 7,
            out_specs=(hbm,) * 4,
            scratch_shapes=[pltpu.VMEM((rows, block), jnp.bfloat16), dma((3, CHUNKS)), dma],
            compiler_params=pltpu.CompilerParams(vmem_limit_bytes=2 * 1024 * 1024),
        )(*held))

    return jax.shard_map(
        shards,
        mesh=mesh,
        in_specs=(P("fs", "tp"), P("fs"), P("fs", "tp"), P("fs", "tp"), P("fs", "tp"), P("tp")),
        out_specs=(P("fs", "tp"), P(None, "tp"), P(None, "tp"), P(None, "tp")),
        check_vma=False,
    )
```

```python
import functools

import jax
import jax.numpy as jnp
from jax import lax
from jax.experimental import pallas as pl
from jax.experimental.pallas import tpu as pltpu
from jax.sharding import PartitionSpec as P

EPS = 1e-06
MESH = pl.DeviceIdType.MESH
P_PART, Q_PART = 0, 1
UP, DOWN, RIGHT, LEFT = 0, 1, 2, 3
CHUNKS = 4


def kernel(
    fs, tp, lines, cols,
    tokens, pre_gain, gate_weight, up_weight, down_weight, post_gain,
    totals, squares, gains_out, gate_out, up_out, down_out,
    staged, gains_row, gains_in, whole, normed, gate, hidden, part, parts_in, powers,
    send_sem, recv_sem, down_recv, stage_sem, gain_sem, tok_send, tok_recv, tok_own,
    rs_send, rs_recv,
):
    weights, outs = (gate_weight, up_weight, down_weight), (gate_out, up_out, down_out)
    depth, width = gate_weight.shape
    half = depth // 2
    rows, block = tokens.shape
    me_fs, me = lax.axis_index("fs"), lax.axis_index("tp")
    z, x = me_fs // cols, lax.rem(me_fs, cols)

    sides = {
        UP: (z < lines - 1, me_fs + cols),
        DOWN: (z > 0, me_fs - cols),
        RIGHT: (x < cols - 1, me_fs + 1),
        LEFT: (x > 0, me_fs - 1),
    }
    peers = [lax.rem(me + j, tp) for j in range(1, tp)]
    corner = jnp.logical_or(z == 0, z == lines - 1)

    def describe(m, which, shard, side, target):
        if m < 2:
            ref = outs[m].at[pl.ds(pl.multiple_of(shard * depth, 16), depth), :]
            landed = recv_sem.at[m, shard]
        else:
            ref = outs[2].at[pl.ds(pl.multiple_of(shard * depth + which * half, 16), half), :]
            landed = down_recv.at[which, shard]
        return pltpu.make_async_remote_copy(
            src_ref=ref, dst_ref=ref, send_sem=send_sem.at[m, side], recv_sem=landed,
            device_id={"fs": target, "tp": me}, device_id_type=MESH,
        )

    def send(m, which, shard, side, extra=None):
        there, target = sides[side]
        cond = there if extra is None else jnp.logical_and(there, extra)

        @pl.when(cond)
        def _():
            describe(m, which, shard, side, target).start()

    def arrive(m, which, shard, cond):
        @pl.when(cond)
        def _():
            describe(m, which, shard, 0, lax.rem(me_fs + 1, fs)).wait_recv()

    def sent(m, side, rows_sent):
        ref = outs[m].at[0:rows_sent, :]
        pltpu.make_async_remote_copy(
            src_ref=ref, dst_ref=ref, send_sem=send_sem.at[m, side], recv_sem=recv_sem.at[0, 0],
            device_id={"fs": lax.rem(me_fs + 1, fs), "tp": me}, device_id_type=MESH,
        ).wait_send()

    barrier = pltpu.get_barrier_semaphore()
    for side in sides:
        there, target = sides[side]

        @pl.when(there)
        def _():
            pl.semaphore_signal(barrier, inc=1, device_id={"fs": target, "tp": me}, device_id_type=MESH)

    for peer in peers:
        pl.semaphore_signal(barrier, inc=1, device_id={"fs": me_fs, "tp": peer}, device_id_type=MESH)

    gain_load = pltpu.make_async_copy(pre_gain, gains_row, gain_sem.at[0])
    gain_load.start()
    size = depth // CHUNKS

    def load(m, c):
        here = pl.ds(c * size, size)
        sem = stage_sem.at[c] if m == 0 else stage_sem.at[CHUNKS + m - 1]
        return pltpu.make_async_copy(weights[m].at[here, :], staged.at[m, here, :], sem)

    for c in range(CHUNKS):
        load(0, c).start()
    own_tokens = pltpu.make_async_copy(tokens, whole.at[me], tok_own)
    post_load = pltpu.make_async_copy(post_gain, gains_out, gain_sem.at[1])
    gain_load.wait()
    gains_in[...] = jnp.transpose(jnp.broadcast_to(gains_row[0:1, :], (128, depth)))

    def cast(m, start, size):
        @pl.loop(start // 16, (start + size) // 16)
        def _(i):
            here = pl.ds(pl.multiple_of(i * 16, 16), 16)
            v = staged[m, here, :]
            if m < 2:
                v = gains_in[here, 0:1] * v
            outs[m][pl.ds(pl.multiple_of(me_fs * depth + i * 16, 16), 16), :] = v.astype(jnp.bfloat16)

    def cast_all(m):
        pltpu.make_async_copy(weights[m], staged.at[m], stage_sem.at[CHUNKS + m - 1]).wait()
        cast(m, 0, depth)

    def token_copy(j):
        return pltpu.make_async_remote_copy(
            src_ref=tokens, dst_ref=whole.at[me], send_sem=tok_send, recv_sem=tok_recv,
            device_id={"fs": me_fs, "tp": peers[j]}, device_id_type=MESH,
        )

    def token_all():
        ref = whole.at[0:tp - 1]
        return pltpu.make_async_remote_copy(
            src_ref=ref, dst_ref=ref, send_sem=tok_send, recv_sem=tok_recv,
            device_id={"fs": me_fs, "tp": peers[0]}, device_id_type=MESH,
        )

    for c in range(CHUNKS):
        load(0, c).wait()
        cast(0, c * size, size)
        if c == 0:
            for m in (1, 2):
                for k in range(CHUNKS):
                    load(m, k).start()
            own_tokens.start()
            post_load.start()
            pl.semaphore_wait(barrier, tp - 1 + sum(there.astype(jnp.int32) for there, _ in sides.values()))
        ref = gate_out.at[pl.ds(pl.multiple_of(me_fs * depth + c * size, 16), size), :]
        for side, (there, target) in sides.items():
            @pl.when(there)
            def _():
                pltpu.make_async_remote_copy(
                    src_ref=ref, dst_ref=ref, send_sem=send_sem.at[0, side], recv_sem=recv_sem.at[0, me_fs],
                    device_id={"fs": target, "tp": me}, device_id_type=MESH,
                ).start()

    for j in range(tp - 1):
        token_copy(j).start()
    cast_all(1)
    for side in sides:
        send(1, Q_PART, me_fs, side)
    cast_all(2)
    for side in (RIGHT, LEFT):
        send(2, P_PART, me_fs, side)

    def normalize():
        own_tokens.wait()
        token_all().wait_recv()
        step = 64

        @pl.loop(0, rows // step)
        def _(i):
            here = pl.ds(pl.multiple_of(i * step, step), step)
            total = jnp.zeros((step, 1), jnp.float32)
            for t in range(tp):
                v = whole[t, here, :].astype(jnp.float32)
                total = total + jnp.sum(v * v, axis=1, keepdims=True)
            scale = lax.rsqrt(total / (tp * block) + EPS)
            for t in range(tp):
                v = whole[t, here, :].astype(jnp.float32)
                normed[here, t * block:(t + 1) * block] = (v * scale).astype(jnp.bfloat16)

    def valid(line):
        return jnp.logical_and(line >= 0, line < lines)

    def around(s):
        return (UP, z - 1 - s), (DOWN, z + 1 + s)

    def along_x(m, which, line, cond=None):
        for r in range(cols - 1):
            for side, column in ((RIGHT, x - 1 - r), (LEFT, x + 1 + r)):
                there = jnp.logical_and(column >= 0, column < cols)
                if cond is not None:
                    there = jnp.logical_and(there, cond)
                arrive(m, which, line * cols + column, there)
                if r < cols - 2:
                    send(m, which, line * cols + column, side, there)

    def along_z(m, s):
        for side, line in around(s):
            there = valid(line)
            shard = line * cols + x
            arrive(m, Q_PART, shard, there)
            if s < lines - 2:
                send(m, Q_PART, shard, side, there)
            if m < 2:
                send(m, Q_PART, shard, RIGHT, there)
                send(m, Q_PART, shard, LEFT, there)

    final = {UP: jnp.minimum(me, lines - 2), DOWN: jnp.maximum(me, 1)}
    next_to_end = {UP: z == lines - 2, DOWN: z == 1}

    def put_off(side, line):
        return jnp.logical_and(next_to_end[side], line == final[side])

    def own_down(s):
        for side, behind in ((UP, z), (DOWN, lines - 1 - z)):
            now = behind <= 1 if s == 0 else behind == s + 1
            send(2, Q_PART, me_fs, side, now)
            now = jnp.logical_and(now, jnp.logical_not(put_off(side, z)))
            for c in range(cols):
                send(2, P_PART, z * cols + lax.rem(x + c, cols), side, now)

    def pass_p(s):
        for side, line in around(s):
            there = jnp.logical_and(valid(line), sides[side][0])
            on = jnp.logical_not(put_off(side, line))
            for c in range(cols):
                shard = line * cols + lax.rem(x + c, cols)
                arrive(2, P_PART, shard, there)
                send(2, P_PART, shard, side, jnp.logical_and(there, on))

    for s in range(lines - 1):
        for m in range(2):
            along_z(m, s)
        if s == 0:
            along_x(2, P_PART, z)
        own_down(s)
        if s == 0:
            normalize()
    for s in range(lines - 1):
        along_z(2, s)

    def in_turn(i):
        return me if i is None else jnp.where(i < me, i, i + 1)

    for i in list(range(lines - 1)) + [None]:
        for side in (RIGHT, LEFT):
            send(2, Q_PART, in_turn(i) * cols + x, side)
    for s in range(lines - 2):
        pass_p(s)
    for side in (UP, DOWN):
        for c in range(cols):
            send(2, P_PART, final[side] * cols + lax.rem(x + c, cols), side, next_to_end[side])

    tile = 256

    def project(m):
        along_x(m, Q_PART, z)
        for s in range(lines - 1):
            for _, line in around(s):
                along_x(m, Q_PART, line, valid(line))

        @pl.loop(0, width // tile)
        def _(i):
            here = pl.ds(pl.multiple_of(i * tile, tile), tile)
            product = jnp.dot(normed[...], outs[m][:, here], preferred_element_type=jnp.float32)
            if m == 0:
                gate[:, here] = product
            else:
                g = gate[:, here]
                hidden[:, here] = (g / (1.0 + jnp.exp(-g)) * product).astype(jnp.bfloat16)

    def share_copy(line, column, which):
        return pltpu.make_async_remote_copy(
            src_ref=part.at[line, column, which], dst_ref=parts_in.at[me, column, which],
            send_sem=rs_send, recv_sem=rs_recv.at[column, which],
            device_id={"fs": me_fs, "tp": line}, device_id_type=MESH,
        )

    def mix(line, column, which):
        here = pl.ds(pl.multiple_of((line * cols + column) * depth + which * half, 16), half)
        product = lax.dot_general(
            hidden[...], outs[2][here, :], (((1,), (1,)), ((), ())), preferred_element_type=jnp.float32
        )
        part[line, column, which] = product.astype(jnp.bfloat16)

        @pl.when(line != me)
        def _():
            share_copy(line, column, which).start()

    def mix_columns(line, which, first, cond=None):
        @pl.loop(first, cols)
        def _(c):
            if cond is None:
                mix(line, lax.rem(x + c, cols), which)
            else:
                pl.when(cond)(lambda: mix(line, lax.rem(x + c, cols), which))

    def shares_in(column, which):
        ref = parts_in.at[0:tp - 1, column, which]
        pltpu.make_async_remote_copy(
            src_ref=ref, dst_ref=ref, send_sem=rs_send, recv_sem=rs_recv.at[column, which],
            device_id={"fs": me_fs, "tp": peers[0]}, device_id_type=MESH,
        ).wait_recv()

    def sum_up(column, which, here):
        total = part[me, column, which, here, :].astype(jnp.float32)
        for peer in peers:
            total = total + parts_in[peer, column, which, here, :].astype(jnp.float32)
        totals[column, which, here, :] = total
        return total

    def add_up(column, which, first=False):
        shares_in(column, which)
        step = 128

        @pl.loop(0, rows // step)
        def _(i):
            here = pl.ds(pl.multiple_of(i * step, step), step)
            total = sum_up(column, which, here)
            powers[here, :] = total * total if first else powers[here, :] + total * total

    project(0)
    project(1)

    @pl.loop(0, lines)
    def _(line):
        mix(line, x, Q_PART)

    @pl.loop(0, lines)
    def _(line):
        mix_columns(line, P_PART, 0, jnp.logical_or(line == z, jnp.logical_not(corner)))

    inward = jnp.where(z == 0, 1, -1)
    last_p = jnp.where(z == 0, final[DOWN], final[UP])
    last_gap = (last_p - z) * inward

    def late_p(n):
        gap = n // cols + 1
        gap = jnp.where(gap < last_gap, gap, jnp.where(gap < lines - 1, gap + 1, last_gap))
        line, column = z + inward * gap, lax.rem(x + lax.rem(n, cols), cols)

        @pl.when(corner)
        def _():
            arrive(2, P_PART, line * cols + column, corner)
            mix(line, column, P_PART)

    def late_q(line):
        along_x(2, Q_PART, line)
        mix_columns(line, Q_PART, 1)

    ends, turns = (lines - 1) * cols, lines
    lead = max(0, ends - turns)

    @pl.loop(0, lead)
    def _(n):
        late_p(n)

    @pl.loop(0, ends - lead - 1)
    def _(n):
        late_p(lead + n)
        late_q(jnp.where(n < me, n, n + 1))

    def all_sent(matrices):
        for m in matrices:
            along = depth if m < 2 else (1 + cols) * half
            across = lines * depth if m < 2 else (lines + 1) * half
            for n in range(1, lines):
                pl.when(z + 1 == n)(lambda: sent(m, UP, n * along))
                pl.when(lines - z == n)(lambda: sent(m, DOWN, n * along))
            for n in range(1, cols):
                pl.when(x + 1 == n)(lambda: sent(m, RIGHT, n * across))
                pl.when(cols - x == n)(lambda: sent(m, LEFT, n * across))

    all_sent((0, 1))
    token_all().wait_send()
    post_load.wait()
    add_up(x, Q_PART, True)
    for c in range(cols - 1):
        add_up(lax.rem(x + c, cols), P_PART)
    together = jnp.logical_and(corner, last_p == me)

    @pl.when(together)
    def _():
        column = lax.rem(x + cols - 1, cols)
        arrive(2, P_PART, me * cols + column, together)
        along_x(2, Q_PART, me)
        for c in range(1, cols - 1):
            mix(me, lax.rem(x + c, cols), Q_PART)
        here = pl.ds(pl.multiple_of((me * cols + column) * depth, 16), depth)
        product = lax.dot_general(
            hidden[...], outs[2][here, :], (((1,), (1,)), ((), ())), preferred_element_type=jnp.float32
        )
        part[me, column, P_PART] = product[:, :half].astype(jnp.bfloat16)
        part[me, column, Q_PART] = product[:, half:].astype(jnp.bfloat16)

    @pl.when(jnp.logical_not(together))
    def _():
        late_p(jnp.int32(ends - 1))
        late_q(me)

    pieces = [(lax.rem(x + cols - 1, cols), P_PART)] + [(lax.rem(x + c, cols), Q_PART) for c in range(1, cols)]
    for column, which in pieces:
        shares_in(column, which)
    step = 128

    @pl.loop(0, rows // step)
    def _(i):
        here = pl.ds(pl.multiple_of(i * step, step), step)
        power = powers[here, :]
        for column, which in pieces:
            total = sum_up(column, which, here)
            power = power + total * total
        square = jnp.sum(power, axis=1, keepdims=True)
        squares[:, here] = jnp.transpose(jnp.broadcast_to(square, (step, 128)))[0:8, :]

    all_sent((2,))
    ref = parts_in.at[0:tp - 1]
    pltpu.make_async_remote_copy(
        src_ref=ref, dst_ref=ref, send_sem=rs_send, recv_sem=rs_recv.at[0, 0],
        device_id={"fs": me_fs, "tp": peers[0]}, device_id_type=MESH,
    ).wait_send()

def write_first(gate_held, up_held, gate_out, up_out, sems):
    copies = []
    for k, (ref, out) in enumerate(((gate_held, gate_out), (up_held, up_out))):
        size = ref.shape[0] // CHUNKS
        for c in range(CHUNKS):
            here = pl.ds(c * size, size)
            copies.append(pltpu.make_async_copy(ref.at[here, :], out.at[here, :], sems.at[k, c]))
    for c in copies:
        c.start()
    for c in copies:
        c.wait()


def write_rest(
    width, tp, totals, gains, down_held, *refs,
):
    squares, (result_out, down_out, result, sems, last) = refs[:tp], refs[tp:]
    copies = []
    for k, (ref, out) in enumerate(((down_held, down_out),)):
        size = ref.shape[0] // CHUNKS
        for c in range(CHUNKS):
            here = pl.ds(c * size, size)
            copies.append(pltpu.make_async_copy(ref.at[here, :], out.at[here, :], sems.at[k, c]))
    for c in copies:
        c.start()
    rows, block = result.shape
    cols, _, _, half = totals.shape
    step = 128

    @pl.loop(0, rows // step)
    def _(i):
        here = pl.ds(pl.multiple_of(i * step, step), step)
        total = squares[0][:, here]
        for other in squares[1:]:
            total = total + other[:, here]
        total = jnp.broadcast_to(total[0:1, :], (128, step))
        scale = lax.rsqrt(jnp.transpose(total)[:, 0:1] / width + EPS)
        for c in range(cols):
            for which in range(2):
                at = slice((2 * c + which) * half, (2 * c + which + 1) * half)
                result[here, at] = (totals[c, which, here, :] * scale * gains[0:1, at]).astype(jnp.bfloat16)

    final = pltpu.make_async_copy(result, result_out, last)
    final.start()
    for c in copies:
        c.wait()
    final.wait()


def solution(mesh):
    fs, tp = mesh.shape["fs"], mesh.shape["tp"]
    lines, cols = tp, fs // tp

    def shards(tokens, pre_gain, gate_weight, up_weight, down_weight, post_gain):
        depth, width = gate_weight.shape
        rows, block = tokens.shape
        hbm = pl.BlockSpec(memory_space=pltpu.HBM)
        vmem = pl.BlockSpec(memory_space=pltpu.VMEM)
        dma = pltpu.SemaphoreType.DMA
        half = depth // 2
        shapes = [(rows, block)] + [(fs * depth, width)] * 3
        held = pl.pallas_call(
            functools.partial(kernel, fs, tp, lines, cols),
            out_shape=(
                pltpu.VMEM((cols, 2, rows, half), jnp.float32),
                pltpu.VMEM((8, rows), jnp.float32),
                pltpu.VMEM((1, block), jnp.float32),
            ) + tuple(pltpu.VMEM(s, jnp.bfloat16) for s in shapes[1:]),
            in_specs=[hbm] * 6,
            out_specs=(vmem,) * 6,
            scratch_shapes=[
                pltpu.VMEM((3, depth, width), jnp.float32),
                pltpu.VMEM((1, depth), jnp.float32),
                pltpu.VMEM((depth, 128), jnp.float32),
                pltpu.VMEM((tp, rows, block), jnp.bfloat16),
                pltpu.VMEM((rows, tp * block), jnp.bfloat16),
                pltpu.VMEM((rows, width), jnp.float32),
                pltpu.VMEM((rows, width), jnp.bfloat16),
                pltpu.VMEM((tp, cols, 2, rows, half), jnp.bfloat16),
                pltpu.VMEM((tp, cols, 2, rows, half), jnp.bfloat16),
                pltpu.VMEM((rows, half), jnp.float32),
                dma((3, 4)), dma((2, fs)), dma((2, fs)), dma((CHUNKS + 2,)), dma((2,)), dma, dma, dma,
                dma, dma((cols, 2)),
            ],
            compiler_params=pltpu.CompilerParams(collective_id=0, has_side_effects=True, vmem_limit_bytes=42 * 1024 * 1024),
        )(tokens, pre_gain[None, :], gate_weight, up_weight, down_weight, post_gain[None, :])
        totals, squares, gains, gate_held, up_held, down_held = held
        others = [lax.ppermute(squares, "tp", [(t, (t + j) % tp) for t in range(tp)]) for j in range(1, tp)]
        gate_ready, up_ready = pl.pallas_call(
            write_first,
            out_shape=tuple(jax.ShapeDtypeStruct(s, jnp.bfloat16) for s in shapes[1:3]),
            in_specs=[vmem] * 2,
            out_specs=(hbm,) * 2,
            scratch_shapes=[dma((2, CHUNKS))],
            compiler_params=pltpu.CompilerParams(vmem_limit_bytes=2 * 1024 * 1024),
        )(gate_held, up_held)
        result, down_ready = pl.pallas_call(
            functools.partial(write_rest, tp * block, tp),
            out_shape=tuple(jax.ShapeDtypeStruct(shapes[k], jnp.bfloat16) for k in (0, 3)),
            in_specs=[vmem] * (3 + tp),
            out_specs=(hbm,) * 2,
            scratch_shapes=[pltpu.VMEM((rows, block), jnp.bfloat16), dma((1, CHUNKS)), dma],
            compiler_params=pltpu.CompilerParams(vmem_limit_bytes=2 * 1024 * 1024),
        )(totals, gains, down_held, squares, *others)
        return result, gate_ready, up_ready, down_ready

    return jax.shard_map(
        shards,
        mesh=mesh,
        in_specs=(P("fs", "tp"), P("fs"), P("fs", "tp"), P("fs", "tp"), P("fs", "tp"), P("tp")),
        out_specs=(P("fs", "tp"), P(None, "tp"), P(None, "tp"), P(None, "tp")),
        check_vma=False,
    )
```

```python
import functools

import jax
import jax.numpy as jnp
from jax import lax
from jax.experimental import pallas as pl
from jax.experimental.pallas import tpu as pltpu
from jax.sharding import PartitionSpec as P

EPS = 1e-06
MESH = pl.DeviceIdType.MESH
P_PART, Q_PART = 0, 1
UP, DOWN, RIGHT, LEFT = 0, 1, 2, 3
CHUNKS = 4


def kernel(
    fs, tp, lines, cols,
    tokens, pre_gain, gate_weight, up_weight, down_weight, post_gain,
    totals, squares, gains_out, gate_out, up_out, down_out,
    staged, gains_row, gains_in, whole, normed, gate, hidden, part, parts_in, powers,
    send_sem, recv_sem, down_recv, stage_sem, gain_sem, tok_send, tok_recv, tok_own,
    rs_send, rs_recv,
):
    weights, outs = (gate_weight, up_weight, down_weight), (gate_out, up_out, down_out)
    depth, width = gate_weight.shape
    half = depth // 2
    rows, block = tokens.shape
    me_fs, me = lax.axis_index("fs"), lax.axis_index("tp")
    z, x = me_fs // cols, lax.rem(me_fs, cols)

    sides = {
        UP: (z < lines - 1, me_fs + cols),
        DOWN: (z > 0, me_fs - cols),
        RIGHT: (x < cols - 1, me_fs + 1),
        LEFT: (x > 0, me_fs - 1),
    }
    peers = [lax.rem(me + j, tp) for j in range(1, tp)]
    corner = jnp.logical_or(z == 0, z == lines - 1)

    def describe(m, which, shard, side, target):
        if m < 2:
            ref = outs[m].at[pl.ds(pl.multiple_of(shard * depth, 16), depth), :]
            landed = recv_sem.at[m, shard]
        else:
            ref = outs[2].at[pl.ds(pl.multiple_of(shard * depth + which * half, 16), half), :]
            landed = down_recv.at[which, shard]
        return pltpu.make_async_remote_copy(
            src_ref=ref, dst_ref=ref, send_sem=send_sem.at[m, side], recv_sem=landed,
            device_id={"fs": target, "tp": me}, device_id_type=MESH,
        )

    def send(m, which, shard, side, extra=None):
        there, target = sides[side]
        cond = there if extra is None else jnp.logical_and(there, extra)

        @pl.when(cond)
        def _():
            describe(m, which, shard, side, target).start()

    def arrive(m, which, shard, cond):
        @pl.when(cond)
        def _():
            describe(m, which, shard, 0, lax.rem(me_fs + 1, fs)).wait_recv()

    def sent(m, side, rows_sent):
        ref = outs[m].at[0:rows_sent, :]
        pltpu.make_async_remote_copy(
            src_ref=ref, dst_ref=ref, send_sem=send_sem.at[m, side], recv_sem=recv_sem.at[0, 0],
            device_id={"fs": lax.rem(me_fs + 1, fs), "tp": me}, device_id_type=MESH,
        ).wait_send()

    gain_load = pltpu.make_async_copy(pre_gain, gains_row, gain_sem.at[0])
    gain_load.start()
    size = depth // CHUNKS

    def load(m, c):
        here = pl.ds(c * size, size)
        sem = stage_sem.at[c] if m == 0 else stage_sem.at[CHUNKS + m - 1]
        return pltpu.make_async_copy(weights[m].at[here, :], staged.at[m, here, :], sem)

    load(0, 0).start()
    barrier = pltpu.get_barrier_semaphore()
    for side in sides:
        there, target = sides[side]

        @pl.when(there)
        def _():
            pl.semaphore_signal(barrier, inc=1, device_id={"fs": target, "tp": me}, device_id_type=MESH)

    for peer in peers:
        pl.semaphore_signal(barrier, inc=1, device_id={"fs": me_fs, "tp": peer}, device_id_type=MESH)

    for c in range(1, CHUNKS):
        load(0, c).start()
    own_tokens = pltpu.make_async_copy(tokens, whole.at[me], tok_own)
    post_load = pltpu.make_async_copy(post_gain, gains_out, gain_sem.at[1])
    gain_load.wait()
    turn = min(128, depth)

    def turn_gains(start):
        gains_in[start:start + turn, :] = jnp.transpose(jnp.broadcast_to(gains_row[0:1, start:start + turn], (128, turn)))

    turn_gains(0)

    def cast(m, start, size):
        @pl.loop(start // 16, (start + size) // 16)
        def _(i):
            here = pl.ds(pl.multiple_of(i * 16, 16), 16)
            v = staged[m, here, :]
            if m < 2:
                v = gains_in[here, 0:1] * v
            outs[m][pl.ds(pl.multiple_of(me_fs * depth + i * 16, 16), 16), :] = v.astype(jnp.bfloat16)

    def cast_all(m):
        pltpu.make_async_copy(weights[m], staged.at[m], stage_sem.at[CHUNKS + m - 1]).wait()
        cast(m, 0, depth)

    def token_copy(j):
        return pltpu.make_async_remote_copy(
            src_ref=tokens, dst_ref=whole.at[me], send_sem=tok_send, recv_sem=tok_recv,
            device_id={"fs": me_fs, "tp": peers[j]}, device_id_type=MESH,
        )

    def token_all():
        ref = whole.at[0:tp - 1]
        return pltpu.make_async_remote_copy(
            src_ref=ref, dst_ref=ref, send_sem=tok_send, recv_sem=tok_recv,
            device_id={"fs": me_fs, "tp": peers[0]}, device_id_type=MESH,
        )

    for c in range(CHUNKS):
        load(0, c).wait()
        if c == 1:
            for start in range(turn, depth, turn):
                turn_gains(start)
        cast(0, c * size, size)
        if c == 0:
            for m in (1, 2):
                for k in range(CHUNKS):
                    load(m, k).start()
            own_tokens.start()
            post_load.start()
            pl.semaphore_wait(barrier, tp - 1 + sum(there.astype(jnp.int32) for there, _ in sides.values()))
        ref = gate_out.at[pl.ds(pl.multiple_of(me_fs * depth + c * size, 16), size), :]
        for side, (there, target) in sides.items():
            @pl.when(there)
            def _():
                pltpu.make_async_remote_copy(
                    src_ref=ref, dst_ref=ref, send_sem=send_sem.at[0, side], recv_sem=recv_sem.at[0, me_fs],
                    device_id={"fs": target, "tp": me}, device_id_type=MESH,
                ).start()

    for j in range(tp - 1):
        token_copy(j).start()
    cast_all(1)
    for side in sides:
        send(1, Q_PART, me_fs, side)
    cast_all(2)
    for side in (RIGHT, LEFT):
        send(2, P_PART, me_fs, side)

    def normalize():
        own_tokens.wait()
        token_all().wait_recv()
        step = 64

        @pl.loop(0, rows // step)
        def _(i):
            here = pl.ds(pl.multiple_of(i * step, step), step)
            total = jnp.zeros((step, 1), jnp.float32)
            for t in range(tp):
                v = whole[t, here, :].astype(jnp.float32)
                total = total + jnp.sum(v * v, axis=1, keepdims=True)
            scale = lax.rsqrt(total / (tp * block) + EPS)
            for t in range(tp):
                v = whole[t, here, :].astype(jnp.float32)
                normed[here, t * block:(t + 1) * block] = (v * scale).astype(jnp.bfloat16)

    def valid(line):
        return jnp.logical_and(line >= 0, line < lines)

    def around(s):
        return (UP, z - 1 - s), (DOWN, z + 1 + s)

    def along_x(m, which, line, cond=None):
        for r in range(cols - 1):
            for side, column in ((RIGHT, x - 1 - r), (LEFT, x + 1 + r)):
                there = jnp.logical_and(column >= 0, column < cols)
                if cond is not None:
                    there = jnp.logical_and(there, cond)
                arrive(m, which, line * cols + column, there)
                if r < cols - 2:
                    send(m, which, line * cols + column, side, there)

    def along_z(m, s):
        for side, line in around(s):
            there = valid(line)
            shard = line * cols + x
            arrive(m, Q_PART, shard, there)
            if s < lines - 2:
                send(m, Q_PART, shard, side, there)
            if m < 2:
                send(m, Q_PART, shard, RIGHT, there)
                send(m, Q_PART, shard, LEFT, there)

    final = {UP: jnp.minimum(me, lines - 2), DOWN: jnp.maximum(me, 1)}
    next_to_end = {UP: z == lines - 2, DOWN: z == 1}

    def put_off(side, line):
        return jnp.logical_and(next_to_end[side], line == final[side])

    def own_down(s):
        for side, behind in ((UP, z), (DOWN, lines - 1 - z)):
            now = behind <= 1 if s == 0 else behind == s + 1
            send(2, Q_PART, me_fs, side, now)
            now = jnp.logical_and(now, jnp.logical_not(put_off(side, z)))
            for c in range(cols):
                send(2, P_PART, z * cols + lax.rem(x + c, cols), side, now)

    def pass_p(s):
        for side, line in around(s):
            there = jnp.logical_and(valid(line), sides[side][0])
            on = jnp.logical_not(put_off(side, line))
            for c in range(cols):
                shard = line * cols + lax.rem(x + c, cols)
                arrive(2, P_PART, shard, there)
                send(2, P_PART, shard, side, jnp.logical_and(there, on))

    for s in range(lines - 1):
        for m in range(2):
            along_z(m, s)
        if s == 0:
            along_x(2, P_PART, z)
        own_down(s)
        if s == 0:
            normalize()
    for s in range(lines - 1):
        along_z(2, s)

    def in_turn(i):
        return me if i is None else jnp.where(i < me, i, i + 1)

    for i in list(range(lines - 1)) + [None]:
        for side in (RIGHT, LEFT):
            send(2, Q_PART, in_turn(i) * cols + x, side)
    for s in range(lines - 2):
        pass_p(s)
    for side in (UP, DOWN):
        for c in range(cols):
            send(2, P_PART, final[side] * cols + lax.rem(x + c, cols), side, next_to_end[side])

    tile = 256

    def project(m):
        along_x(m, Q_PART, z)
        for s in range(lines - 1):
            for _, line in around(s):
                along_x(m, Q_PART, line, valid(line))

        @pl.loop(0, width // tile)
        def _(i):
            here = pl.ds(pl.multiple_of(i * tile, tile), tile)
            product = jnp.dot(normed[...], outs[m][:, here], preferred_element_type=jnp.float32)
            if m == 0:
                gate[:, here] = product
            else:
                g = gate[:, here]
                hidden[:, here] = (g / (1.0 + jnp.exp(-g)) * product).astype(jnp.bfloat16)

    def share_copy(line, column, which):
        return pltpu.make_async_remote_copy(
            src_ref=part.at[line, column, which], dst_ref=parts_in.at[me, column, which],
            send_sem=rs_send, recv_sem=rs_recv.at[column, which],
            device_id={"fs": me_fs, "tp": line}, device_id_type=MESH,
        )

    def mix(line, column, which):
        here = pl.ds(pl.multiple_of((line * cols + column) * depth + which * half, 16), half)
        product = lax.dot_general(
            hidden[...], outs[2][here, :], (((1,), (1,)), ((), ())), preferred_element_type=jnp.float32
        )
        part[line, column, which] = product.astype(jnp.bfloat16)

        @pl.when(line != me)
        def _():
            share_copy(line, column, which).start()

    def mix_columns(line, which, first, cond=None):
        @pl.loop(first, cols)
        def _(c):
            if cond is None:
                mix(line, lax.rem(x + c, cols), which)
            else:
                pl.when(cond)(lambda: mix(line, lax.rem(x + c, cols), which))

    def shares_in(column, which):
        ref = parts_in.at[0:tp - 1, column, which]
        pltpu.make_async_remote_copy(
            src_ref=ref, dst_ref=ref, send_sem=rs_send, recv_sem=rs_recv.at[column, which],
            device_id={"fs": me_fs, "tp": peers[0]}, device_id_type=MESH,
        ).wait_recv()

    def sum_up(column, which, here):
        total = part[me, column, which, here, :].astype(jnp.float32)
        for peer in peers:
            total = total + parts_in[peer, column, which, here, :].astype(jnp.float32)
        totals[column, which, here, :] = total
        return total

    def add_up(column, which, first=False):
        shares_in(column, which)
        step = 128

        @pl.loop(0, rows // step)
        def _(i):
            here = pl.ds(pl.multiple_of(i * step, step), step)
            total = sum_up(column, which, here)
            powers[here, :] = total * total if first else powers[here, :] + total * total

    project(0)
    project(1)

    @pl.loop(0, lines)
    def _(line):
        mix(line, x, Q_PART)

    @pl.loop(0, lines)
    def _(line):
        mix_columns(line, P_PART, 0, jnp.logical_or(line == z, jnp.logical_not(corner)))

    inward = jnp.where(z == 0, 1, -1)
    last_p = jnp.where(z == 0, final[DOWN], final[UP])
    last_gap = (last_p - z) * inward

    def late_p(n):
        gap = n // cols + 1
        gap = jnp.where(gap < last_gap, gap, jnp.where(gap < lines - 1, gap + 1, last_gap))
        line, column = z + inward * gap, lax.rem(x + lax.rem(n, cols), cols)

        @pl.when(corner)
        def _():
            arrive(2, P_PART, line * cols + column, corner)
            mix(line, column, P_PART)

    def late_q(line):
        along_x(2, Q_PART, line)
        mix_columns(line, Q_PART, 1)

    ends, turns = (lines - 1) * cols, lines
    lead = max(0, ends - turns)

    @pl.loop(0, lead)
    def _(n):
        late_p(n)

    @pl.loop(0, ends - lead - 1)
    def _(n):
        late_p(lead + n)
        late_q(jnp.where(n < me, n, n + 1))

    def all_sent(matrices):
        for m in matrices:
            along = depth if m < 2 else (1 + cols) * half
            across = lines * depth if m < 2 else (lines + 1) * half
            for n in range(1, lines):
                pl.when(z + 1 == n)(lambda: sent(m, UP, n * along))
                pl.when(lines - z == n)(lambda: sent(m, DOWN, n * along))
            for n in range(1, cols):
                pl.when(x + 1 == n)(lambda: sent(m, RIGHT, n * across))
                pl.when(cols - x == n)(lambda: sent(m, LEFT, n * across))

    all_sent((0, 1))
    token_all().wait_send()
    post_load.wait()
    add_up(x, Q_PART, True)
    for c in range(cols - 1):
        add_up(lax.rem(x + c, cols), P_PART)
    together = jnp.logical_and(corner, last_p == me)

    @pl.when(together)
    def _():
        column = lax.rem(x + cols - 1, cols)
        arrive(2, P_PART, me * cols + column, together)
        along_x(2, Q_PART, me)
        for c in range(1, cols - 1):
            mix(me, lax.rem(x + c, cols), Q_PART)
        here = pl.ds(pl.multiple_of((me * cols + column) * depth, 16), depth)
        product = lax.dot_general(
            hidden[...], outs[2][here, :], (((1,), (1,)), ((), ())), preferred_element_type=jnp.float32
        )
        part[me, column, P_PART] = product[:, :half].astype(jnp.bfloat16)
        part[me, column, Q_PART] = product[:, half:].astype(jnp.bfloat16)

    @pl.when(jnp.logical_not(together))
    def _():
        late_p(jnp.int32(ends - 1))
        late_q(me)

    pieces = [(lax.rem(x + cols - 1, cols), P_PART)] + [(lax.rem(x + c, cols), Q_PART) for c in range(1, cols)]
    for column, which in pieces:
        shares_in(column, which)
    step = 128

    @pl.loop(0, rows // step)
    def _(i):
        here = pl.ds(pl.multiple_of(i * step, step), step)
        power = powers[here, :]
        for column, which in pieces:
            total = sum_up(column, which, here)
            power = power + total * total
        square = jnp.sum(power, axis=1, keepdims=True)
        squares[:, here] = jnp.transpose(jnp.broadcast_to(square, (step, 128)))[0:8, :]

    all_sent((2,))
    ref = parts_in.at[0:tp - 1]
    pltpu.make_async_remote_copy(
        src_ref=ref, dst_ref=ref, send_sem=rs_send, recv_sem=rs_recv.at[0, 0],
        device_id={"fs": me_fs, "tp": peers[0]}, device_id_type=MESH,
    ).wait_send()

def write_first(gate_held, up_held, gate_out, up_out, sems):
    copies = []
    for k, (ref, out) in enumerate(((gate_held, gate_out), (up_held, up_out))):
        size = ref.shape[0] // CHUNKS
        for c in range(CHUNKS):
            here = pl.ds(c * size, size)
            copies.append(pltpu.make_async_copy(ref.at[here, :], out.at[here, :], sems.at[k]))
    for c in copies:
        c.start()
    for k, (ref, out) in enumerate(((gate_held, gate_out), (up_held, up_out))):
        pltpu.make_async_copy(ref, out, sems.at[k]).wait()


def write_rest(
    width, tp, totals, gains, down_held, *refs,
):
    squares, (result_out, down_out, result, sems, last) = refs[:tp], refs[tp:]
    copies = []
    for k, (ref, out) in enumerate(((down_held, down_out),)):
        size = ref.shape[0] // CHUNKS
        for c in range(CHUNKS):
            here = pl.ds(c * size, size)
            copies.append(pltpu.make_async_copy(ref.at[here, :], out.at[here, :], sems.at[k]))
    for c in copies:
        c.start()
    rows, block = result.shape
    cols, _, _, half = totals.shape
    step = 128

    @pl.loop(0, rows // step)
    def _(i):
        here = pl.ds(pl.multiple_of(i * step, step), step)
        total = squares[0][:, here]
        for other in squares[1:]:
            total = total + other[:, here]
        total = jnp.broadcast_to(total[0:1, :], (128, step))
        scale = lax.rsqrt(jnp.transpose(total)[:, 0:1] / width + EPS)
        for c in range(cols):
            for which in range(2):
                at = slice((2 * c + which) * half, (2 * c + which + 1) * half)
                result[here, at] = (totals[c, which, here, :] * scale * gains[0:1, at]).astype(jnp.bfloat16)

    final = pltpu.make_async_copy(result, result_out, last)
    final.start()
    pltpu.make_async_copy(down_held, down_out, sems.at[0]).wait()
    final.wait()


def solution(mesh):
    fs, tp = mesh.shape["fs"], mesh.shape["tp"]
    lines, cols = tp, fs // tp

    def shards(tokens, pre_gain, gate_weight, up_weight, down_weight, post_gain):
        depth, width = gate_weight.shape
        rows, block = tokens.shape
        hbm = pl.BlockSpec(memory_space=pltpu.HBM)
        vmem = pl.BlockSpec(memory_space=pltpu.VMEM)
        dma = pltpu.SemaphoreType.DMA
        half = depth // 2
        shapes = [(rows, block)] + [(fs * depth, width)] * 3
        held = pl.pallas_call(
            functools.partial(kernel, fs, tp, lines, cols),
            out_shape=(
                pltpu.VMEM((cols, 2, rows, half), jnp.float32),
                pltpu.VMEM((8, rows), jnp.float32),
                pltpu.VMEM((1, block), jnp.float32),
            ) + tuple(pltpu.VMEM(s, jnp.bfloat16) for s in shapes[1:]),
            in_specs=[hbm] * 6,
            out_specs=(vmem,) * 6,
            scratch_shapes=[
                pltpu.VMEM((3, depth, width), jnp.float32),
                pltpu.VMEM((1, depth), jnp.float32),
                pltpu.VMEM((depth, 128), jnp.float32),
                pltpu.VMEM((tp, rows, block), jnp.bfloat16),
                pltpu.VMEM((rows, tp * block), jnp.bfloat16),
                pltpu.VMEM((rows, width), jnp.float32),
                pltpu.VMEM((rows, width), jnp.bfloat16),
                pltpu.VMEM((tp, cols, 2, rows, half), jnp.bfloat16),
                pltpu.VMEM((tp, cols, 2, rows, half), jnp.bfloat16),
                pltpu.VMEM((rows, half), jnp.float32),
                dma((3, 4)), dma((2, fs)), dma((2, fs)), dma((CHUNKS + 2,)), dma((2,)), dma, dma, dma,
                dma, dma((cols, 2)),
            ],
            compiler_params=pltpu.CompilerParams(collective_id=0, has_side_effects=True, vmem_limit_bytes=42 * 1024 * 1024),
        )(tokens, pre_gain[None, :], gate_weight, up_weight, down_weight, post_gain[None, :])
        totals, squares, gains, gate_held, up_held, down_held = held
        others = [lax.ppermute(squares, "tp", [(t, (t + j) % tp) for t in range(tp)]) for j in range(1, tp)]
        gate_ready, up_ready = pl.pallas_call(
            write_first,
            out_shape=tuple(jax.ShapeDtypeStruct(s, jnp.bfloat16) for s in shapes[1:3]),
            in_specs=[vmem] * 2,
            out_specs=(hbm,) * 2,
            scratch_shapes=[dma((2,))],
            compiler_params=pltpu.CompilerParams(vmem_limit_bytes=2 * 1024 * 1024),
        )(gate_held, up_held)
        result, down_ready = pl.pallas_call(
            functools.partial(write_rest, tp * block, tp),
            out_shape=tuple(jax.ShapeDtypeStruct(shapes[k], jnp.bfloat16) for k in (0, 3)),
            in_specs=[vmem] * (3 + tp),
            out_specs=(hbm,) * 2,
            scratch_shapes=[pltpu.VMEM((rows, block), jnp.bfloat16), dma((1,)), dma],
            compiler_params=pltpu.CompilerParams(vmem_limit_bytes=2 * 1024 * 1024),
        )(totals, gains, down_held, squares, *others)
        return result, gate_ready, up_ready, down_ready

    return jax.shard_map(
        shards,
        mesh=mesh,
        in_specs=(P("fs", "tp"), P("fs"), P("fs", "tp"), P("fs", "tp"), P("fs", "tp"), P("tp")),
        out_specs=(P("fs", "tp"), P(None, "tp"), P(None, "tp"), P(None, "tp")),
        check_vma=False,
    )
```
